32 devices in a mesh: sp: 8 (over z, x), dp: 4 (over y, core).
Axes of the slice: x: 2, y: 2, z: 4, core: 2. Of those that a mesh axis runs over, the one named last changes fastest.
Arguments:
- tokens: bfloat16 [4, 3072, 2048], P('dp', 'sp'), may hold values from -6 to 6
- q_weight: bfloat16 [2048, 1024], P(('sp', 'dp')), may hold values from -0.13258252 to 0.13258252
- k_weight: bfloat16 [2048, 256], P(('sp', 'dp')), may hold values from -0.13258252 to 0.13258252
- v_weight: bfloat16 [2048, 256], P(('sp', 'dp')), may hold values from -0.125 to 0.125
- out_weight: bfloat16 [1024, 2048], P(None, ('sp', 'dp')), may hold values from -6 to 6
- q_gain: float32 [64], replicated, may hold values from 0.5 to 8
- k_gain: float32 [64], replicated, may hold values from 0.5 to 8
Outputs:
- mixed: bfloat16 [4, 3072, 2048], P('dp', 'sp')
The draws below stay inside these ranges and needn't reach their ends.
All inputs are finite; a program needn't handle non-finite values.
Results may differ from the reference program's by a relative error of at most 0.0055.
The reference program's roundings to bfloat16 on the way (of `values`, `shares` and `attended`) count: a program that leaves them out, or rounds other values in their place, can miss the bound.
Values may be sent and summed in bfloat16 or wider, within the bound.
A program may use at most 128 MiB of HBM per device.

```python
import math
import jax
import jax.numpy as jnp
from jax import lax

D = 2048
Q_HEADS = 16
KV_HEADS = 4
HEAD_DIM = 64
GRID_W = 64
GROUP = 4
SEQ = 3072
BATCH = 4


def draw_pair(key):
    query_draw = jnp.clip(jax.random.normal(jax.random.fold_in(key, 11), (D, Q_HEADS * HEAD_DIM), jnp.float32), -6.0, 6.0) / math.sqrt(D)
    key_draw = jnp.clip(jax.random.normal(jax.random.fold_in(key, 12), (D, KV_HEADS * HEAD_DIM), jnp.float32), -6.0, 6.0) / math.sqrt(D)
    return (query_draw, key_draw)


def draw_q_weight(key, part):
    return draw_pair(key)[0].astype(jnp.bfloat16)


def draw_k_weight(key, part):
    return draw_pair(key)[1].astype(jnp.bfloat16)


def draw_gain(key):
    return 1.0 + 0.18 * jnp.clip(jax.random.normal(key, (HEAD_DIM,), jnp.float32), -2.5, 2.5)


def draw_q_gain(key, part):
    return draw_gain(jax.random.fold_in(key, 21))


def draw_k_gain(key, part):
    return draw_gain(jax.random.fold_in(key, 22))


def steps_of(rng, dims, shards, smallest, largest):
    def one(axis_at, parts):
        steps = jax.random.uniform(jax.random.fold_in(jax.random.fold_in(rng, 6), axis_at), (parts,), jnp.float32, smallest / len(shards), largest / len(shards))
        return jnp.repeat(jnp.exp(steps), dims[axis_at] // parts).reshape((-1,) + (1,) * (len(dims) - axis_at - 1))

    gain = one(*shards[0])
    for cut in shards[1:]:
        gain = gain * one(*cut)
    return gain


def noise(rng, shape, scale, limit, pieces=(), kind=jnp.bfloat16):
    array = jax.random.normal(rng, shape, jnp.float32) * scale
    if len(pieces) > 0:
        array = steps_of(rng, shape, pieces, -0.22, 0.18) * array
    return jnp.clip(array, min=-limit, max=limit).astype(kind)


def setup_inputs(seed: int = 0) -> dict:
    key_list = jax.random.split(jax.random.key(seed), 8)
    return {
        "tokens": noise(key_list[0], (BATCH, SEQ, D), 1.0, 6.0, ((0, 4), (1, 8))),
        "q_weight": draw_q_weight(jax.random.fold_in(key_list[7], 71), 0),
        "k_weight": draw_k_weight(jax.random.fold_in(key_list[7], 71), 0),
        "v_weight": noise(key_list[3], (D, KV_HEADS * HEAD_DIM), D ** -0.5, 0.125, ((0, 32),)),
        "out_weight": noise(key_list[4], (Q_HEADS * HEAD_DIM, D), (32.0 / (Q_HEADS * HEAD_DIM) ** 0.5), 6.0, ((1, 32),)),
        "q_gain": draw_q_gain(jax.random.fold_in(key_list[7], 71), 0),
        "k_gain": draw_k_gain(jax.random.fold_in(key_list[7], 71), 0),
    }


epsilon = 1e-06
rope_base = 10000.0

def normalize(tensor, gain_vec):
    mean_sq = lax.optimization_barrier(jnp.mean(tensor * tensor, axis=-1, keepdims=True))
    return tensor * lax.rsqrt(mean_sq + epsilon) * gain_vec.astype(jnp.float32)

def rotate(tensor, offset):
    row_count = tensor.shape[0]
    head_width = tensor.shape[2]
    quarter = head_width // 4
    half_width = head_width // 2
    positions = jnp.arange(row_count, dtype=jnp.int32) + offset
    frequency = rope_base ** (-jnp.arange(quarter, dtype=jnp.float32) / quarter)

    def rotate_pair(segment, coords):
        angles = coords.astype(jnp.float32)[:, None] * frequency[None, :]
        cosine = jnp.cos(angles)[:, None, :]
        sine_val = jnp.sin(angles)[:, None, :]
        low_half = segment[..., :quarter]
        high_half = segment[..., quarter:]
        return jnp.concatenate([low_half * cosine - high_half * sine_val, high_half * cosine + low_half * sine_val], axis=-1)
    return jnp.concatenate([rotate_pair(tensor[..., :half_width], positions // GRID_W), rotate_pair(tensor[..., half_width:], positions % GRID_W)], axis=-1)

def attend(query_rows, key_rows, value_rows):
    row_count, head_width = query_rows.shape
    block_rows = math.gcd(row_count, 512)
    score_scale = head_width ** (-0.5)

    def attend_block(segment):
        scores = lax.dot_general(segment, key_rows, (((1,), (1,)), ((), ())), preferred_element_type=jnp.float32) * score_scale
        row_max = lax.optimization_barrier(jnp.max(scores, axis=-1, keepdims=True))
        weights = jnp.exp(scores - row_max)
        shares = (weights / lax.optimization_barrier(jnp.sum(weights, axis=-1, keepdims=True))).astype(jnp.bfloat16)
        return jnp.dot(shares, value_rows, preferred_element_type=jnp.float32).astype(jnp.bfloat16)
    blocks = query_rows.reshape(row_count // block_rows, block_rows, head_width)
    return lax.map(attend_block, blocks).reshape(row_count, head_width)

def reference(tokens, q_weight, k_weight, v_weight, out_weight, q_gain, k_gain):

    def sequence_out(rows_in):
        seq_len = rows_in.shape[0]
        query_raw = jnp.dot(rows_in, q_weight, preferred_element_type=jnp.float32).reshape(seq_len, Q_HEADS, HEAD_DIM)
        key_raw = jnp.dot(rows_in, k_weight, preferred_element_type=jnp.float32).reshape(seq_len, KV_HEADS, HEAD_DIM)
        value_raw = jnp.dot(rows_in, v_weight, preferred_element_type=jnp.float32).reshape(seq_len, KV_HEADS, HEAD_DIM)
        queries = rotate(normalize(query_raw, q_gain), 0).astype(jnp.bfloat16)
        keys = rotate(normalize(key_raw, k_gain), 0).astype(jnp.bfloat16)
        values = value_raw.astype(jnp.bfloat16)
        q_major = jnp.transpose(queries, (1, 0, 2))
        k_major = jnp.transpose(keys, (1, 0, 2))
        v_major = jnp.transpose(values, (1, 0, 2))

        def head_out(head_index):
            kv_index = head_index // GROUP
            q_rows = lax.dynamic_index_in_dim(q_major, head_index, 0, keepdims=False)
            k_rows = lax.dynamic_index_in_dim(k_major, kv_index, 0, keepdims=False)
            v_rows = lax.dynamic_index_in_dim(v_major, kv_index, 0, keepdims=False)
            return attend(q_rows, k_rows, v_rows)
        heads_done = lax.map(head_out, jnp.arange(Q_HEADS, dtype=jnp.int32))
        attended = jnp.transpose(heads_done, (1, 0, 2)).reshape(seq_len, Q_HEADS * HEAD_DIM)
        return jnp.dot(attended, out_weight, preferred_element_type=jnp.float32).astype(jnp.bfloat16)
    return lax.map(sequence_out, tokens)
```

```python
import functools
import math

import jax
import jax.numpy as jnp
from jax import lax
from jax.experimental import pallas as pl
from jax.experimental.pallas import tpu as pltpu
from jax.sharding import PartitionSpec as P

GRID_W = 64
CORES = 2
epsilon = 1e-06
rope_base = 10000.0
VMEM_BYTES = 60 * 1024 * 1024


class Net:
    def __init__(self, dims):
        self.zs, self.xs, self.ys = dims
        sp, dp = lax.axis_index("sp"), lax.axis_index("dp")
        self.z, self.x = sp // self.xs, sp % self.xs
        self.y, self.c = dp // CORES, dp % CORES
        self.ox, self.oy, self.oc = 1 - self.x, 1 - self.y, 1 - self.c

    def at(self, z=None, x=None, y=None, c=None):
        z = self.z if z is None else z
        x = self.x if x is None else x
        y = self.y if y is None else y
        c = self.c if c is None else c
        return {"sp": z * self.xs + x, "dp": y * CORES + c}

    def near(self, k):
        below, above = self.z, self.zs - 1 - self.z
        both = jnp.minimum(below, above)
        inner = k <= 2 * both
        far = jnp.where(above > below, 1, -1)
        sign = jnp.where(inner, jnp.where(k % 2 == 1, 1, -1), far)
        return self.z + sign * jnp.where(inner, (k + 1) // 2, k - both)


def remote(src, dst, send, recv, where):
    return pltpu.make_async_remote_copy(
        src_ref=src,
        dst_ref=dst,
        send_sem=send,
        recv_sem=recv,
        device_id=where,
        device_id_type=pl.DeviceIdType.MESH,
    )


class Gather:
    def __init__(self, net, buf, sems):
        self.net, self.buf = net, buf
        self.zs, self.zr, self.xs, self.xr, self.ys, self.yr, self.cs, self.cr = sems

    def block(self, k, kind, c=None):
        net = self.net
        x = net.ox if kind % 2 else net.x
        y = net.oy if kind // 2 else net.y
        return self.buf.at[net.near(k), x, y, net.c if c is None else c]

    def over_z(self, k):
        net, b = self.net, self.block(0, 0)
        return remote(b, b, self.zs.at[k - 1], self.zr.at[net.z], net.at(z=net.near(k)))

    def from_z(self, k):
        net, b = self.net, self.block(k, 0)
        return remote(b, b, self.zs.at[k - 1], self.zr.at[net.near(k)], net.at(z=net.near(k)))

    def over_x(self, k, arriving=False):
        b = self.block(k, 1 if arriving else 0)
        return remote(b, b, self.xs.at[k], self.xr.at[k], self.net.at(x=self.net.ox))

    def over_y(self, kind, k, arriving=False):
        b = self.block(k, kind + 2 if arriving else kind)
        return remote(b, b, self.ys.at[kind, k], self.yr.at[kind, k], self.net.at(y=self.net.oy))

    def over_c(self, kind, k, arriving=False):
        b = self.block(k, kind, self.net.oc if arriving else None)
        return remote(b, b, self.cs.at[kind, k], self.cr.at[kind, k], self.net.at(c=self.net.oc))

    def spread(self, k):
        self.over_y(0, k).start()
        self.over_x(k).start()
        self.over_c(0, k).start()

    def start(self):
        for k in range(1, self.net.zs):
            self.over_z(k).start()
        self.spread(0)

    def pass_z(self, k):
        self.from_z(k).wait_recv()
        self.spread(k)

    def pass_x(self, k):
        self.over_x(k, True).wait_recv()
        self.over_y(1, k).start()
        self.over_c(1, k).start()

    def pass_y(self, kind, k):
        self.over_y(kind, k, True).wait_recv()
        self.over_c(kind + 2, k).start()

    def finish(self):
        for k in range(self.net.zs):
            for kind in range(4):
                self.over_c(kind, k, True).wait_recv()

    def drain(self):
        for k in range(self.net.zs):
            if k:
                self.over_z(k).wait_send()
            self.over_x(k).wait_send()
            for kind in range(2):
                self.over_y(kind, k).wait_send()
            for kind in range(4):
                self.over_c(kind, k).wait_send()


class Exchange:
    def __init__(self, net, k_buf, v_buf, head_width, sems):
        self.net, self.bufs, self.head_width = net, (k_buf, v_buf), head_width
        self.zs, self.zr, self.xs, self.xr = sems

    def block(self, i, z, x):
        if i == 0:
            return self.bufs[0].at[z, x]
        return self.bufs[1].at[z, x, :, : self.head_width]

    def over_z(self, i, k):
        net = self.net
        b = self.block(i, net.z, net.x)
        return remote(b, b, self.zs.at[i, k - 1], self.zr.at[i, net.z], net.at(z=net.near(k)))

    def from_z(self, i, k):
        net = self.net
        z = net.near(k)
        b = self.block(i, z, net.x)
        return remote(b, b, self.zs.at[i, k - 1], self.zr.at[i, z], net.at(z=z))

    def over_x(self, i, k, arriving=False):
        net = self.net
        b = self.block(i, net.near(k), net.ox if arriving else net.x)
        return remote(b, b, self.xs.at[i, k], self.xr.at[i, k], net.at(x=net.ox))

    def send_z(self, k):
        for i in range(2):
            self.over_z(i, k).start()

    def send_x(self, k):
        for i in range(2):
            self.over_x(i, k).start()

    def pass_z(self, k):
        for i in range(2):
            self.from_z(i, k).wait_recv()
            self.over_x(i, k).start()

    def arrived(self, k):
        for i in range(2):
            self.over_x(i, k, True).wait_recv()

    def drain(self):
        for k in range(self.net.zs):
            for i in range(2):
                if k:
                    self.over_z(i, k).wait_send()
                self.over_x(i, k).wait_send()


def greet(net):
    barrier = pltpu.get_barrier_semaphore()
    others = [net.at(x=net.ox), net.at(y=net.oy), net.at(c=net.oc)]
    others += [net.at(z=net.near(k)) for k in range(1, net.zs)]
    for where in others:
        pl.semaphore_signal(barrier, inc=1, device_id=where, device_id_type=pl.DeviceIdType.MESH)
    pl.semaphore_wait(barrier, len(others))


def layer_kernel(
    dims, group, scale, head_width, tok_hbm, qw_ref, kw_ref, vw_ref, ow_ref, qg_ref, kg_ref,
    out_ref, tok_ref, wkv, wq, wo, q_ref, k_buf, v_buf, acc_ref, max_ref, att_ref,
    cos_ref, sin_ref, tok_sem, *sems
):
    net = Net(dims)
    rows, depth = tok_ref.shape
    pair = 2 * head_width
    kv_width = kw_ref.shape[1]
    groups = kv_width // head_width
    q_width = qw_ref.shape[1]
    width = 4 * head_width
    load = pltpu.make_async_copy(tok_hbm, tok_ref, tok_sem)
    load.start()
    me = (net.z, net.x, net.y, net.c)
    wkv[me + (slice(None), slice(0, kv_width))] = kw_ref[...]
    wkv[me + (slice(None), slice(kv_width, 2 * kv_width))] = vw_ref[...]
    wq[me] = qw_ref[...]
    wo[me] = ow_ref[...]
    kv_w, q_w, o_w = (
        Gather(net, buf, sems[8 * i : 8 * i + 8]) for i, buf in enumerate((wkv, wq, wo))
    )
    kv = Exchange(net, k_buf, v_buf, head_width, sems[24:])
    steps = net.zs
    greet(net)
    kv_w.start()
    q_w.start()

    lane = lax.broadcasted_iota(jnp.int32, (rows, pair), 1)
    at = lax.broadcasted_iota(jnp.int32, (rows, pair), 0) + (net.z * net.xs + net.x) * rows
    quarter = head_width // 4
    power = (lane % quarter).astype(jnp.float32) * (-math.log(rope_base) / quarter)
    spot = jnp.where(lane % head_width < 2 * quarter, at // GRID_W, at % GRID_W)
    angle = spot.astype(jnp.float32) * jnp.exp(power)
    first = lane % (2 * quarter) < quarter
    cos_ref[...] = jnp.cos(angle)
    sin_ref[...] = jnp.where(first, -jnp.sin(angle), jnp.sin(angle))

    q_ref[...] = jnp.zeros_like(q_ref)
    acc_ref[...] = jnp.zeros_like(acc_ref)
    max_ref[...] = jnp.full_like(max_ref, -jnp.inf)
    tail = v_buf.shape[3] - head_width
    v_buf[:, :, :, head_width:] = jnp.ones(v_buf.shape[:3] + (tail, rows), v_buf.dtype)
    load.wait()

    r = lax.broadcasted_iota(jnp.int32, (2 * width, width), 0) % width // head_width
    c = lax.broadcasted_iota(jnp.int32, (2 * width, width), 1) // head_width
    averager = jnp.where(r == c, 1.0 / head_width, 0.0).astype(jnp.bfloat16)
    wide_first = jnp.concatenate([first, first], axis=1)

    def twice(ref):
        return jnp.concatenate([ref[...]] * 2, axis=1)

    def product(buf, at):
        w = buf[:, :, :, :, :, at : at + width].reshape(depth, width)
        return jnp.dot(tok_ref[...], w, preferred_element_type=jnp.float32)

    def halves(t):
        high = t.astype(jnp.bfloat16)
        return high, (t - high.astype(jnp.float32)).astype(jnp.bfloat16)

    def turned(t, gain_ref):
        gain = jnp.concatenate([gain_ref[...]] * 4, axis=1)
        mean_sq = jnp.dot(
            jnp.concatenate(halves(t * t), axis=1), averager, preferred_element_type=jnp.float32
        )
        t = t * lax.rsqrt(mean_sq + epsilon) * gain
        other = jnp.where(
            wide_first, pltpu.roll(t, width - quarter, 1), pltpu.roll(t, quarter, 1)
        )
        return t * twice(cos_ref) + other * twice(sin_ref)

    for k in range(1, steps):
        kv_w.pass_z(k)
    for k in range(steps):
        kv_w.pass_x(k)
    for k in range(1, steps):
        q_w.pass_z(k)
    for k in range(steps):
        kv_w.pass_y(0, k)
    for k in range(steps):
        kv_w.pass_y(1, k)
    kv_w.finish()
    for j in range(kv_width // width):
        cols = slice(j * width, (j + 1) * width)
        k_buf[net.z, net.x, :, cols] = turned(product(wkv, j * width), kg_ref).astype(k_buf.dtype)
        v = product(wkv, kv_width + j * width).T.astype(v_buf.dtype)
        for i in range(width // head_width):
            v_buf[net.z, net.x, j * (width // head_width) + i, :head_width] = v[
                i * head_width : (i + 1) * head_width
            ]
    kv.send_z(1)
    kv.send_x(0)
    for k in range(2, steps):
        kv.send_z(k)
    for k in range(steps):
        q_w.pass_x(k)
    o_w.start()
    for k in range(steps):
        q_w.pass_y(0, k)
    kv.pass_z(1)
    for k in range(steps):
        q_w.pass_y(1, k)
    q_w.finish()

    for j in range(q_width // width):
        q = turned(product(wq, j * width), qg_ref).astype(jnp.bfloat16).astype(jnp.float32)
        q = (q * (scale * math.log2(math.e))).T
        g = j
        base = (g % 2) * head_width
        for i, part in enumerate(halves(q)):
            for n in range(group):
                q_ref[
                    g, i * pair + base : i * pair + base + head_width, n * rows : (n + 1) * rows
                ] = part[n * head_width : (n + 1) * head_width]

    chunk = width
    keys_now = net.xs * rows
    chunks = group * rows // chunk

    def attend(k, g):
        z = net.near(k)
        keys = k_buf[z, :, :, pl.ds(pl.multiple_of(g // 2 * pair, pair), pair)]
        keys = keys.reshape(keys_now, pair)
        keys = jnp.concatenate([keys, keys], axis=1)
        values = jnp.concatenate([v_buf[z, x, g] for x in range(net.xs)], axis=1)
        cols = [slice(n * chunk, (n + 1) * chunk) for n in range(chunks)]
        scores = [
            jnp.dot(keys, q_ref[g, :, at], preferred_element_type=jnp.float32) for at in cols
        ]
        for at, s in zip(cols, scores):
            old = max_ref[g, :, at]
            top = jnp.maximum(old, jnp.max(s, axis=0, keepdims=True))
            p = jnp.exp2(s - top).astype(values.dtype)
            max_ref[g, :, at] = top
            acc_ref[g, :, at] = acc_ref[g, :, at] * jnp.exp2(old - top) + jnp.dot(
                values, p, preferred_element_type=jnp.float32
            )

    events = {t: [] for t in range(steps * groups)}
    kv.arrived(0)
    for k in range(2, steps):
        events[(k - 2) * groups + 1].append((kv.pass_z, k))
    for k in range(1, steps):
        events[k * groups].append((kv.arrived, k))
        events[2 * groups - 2 + k].append((o_w.pass_z, k))
    for k in range(steps):
        events[2 * groups + 2 + k].append((o_w.pass_x, k))
        events[3 * groups].append((o_w.pass_y, 0, k))

    def step(t, carry):
        k, g = t // groups, t % groups
        for when, todo in events.items():
            if todo:

                @pl.when(t == when)
                def _():
                    for act, *where in todo:
                        act(*where)

        attend(k, g)
        return carry

    lax.fori_loop(0, steps * groups, step, 0)

    for g in range(groups):
        for n in range(0, group, 2):
            parts = []
            for i in (n, n + 1):
                cols = slice(i * rows, (i + 1) * rows)
                total = acc_ref[g, head_width : head_width + 1, cols]
                parts.append(acc_ref[g, :head_width, cols] / total)
            at = (g * group + n) * head_width
            att_ref[:, at : at + pair] = jnp.concatenate(parts, axis=0).T.astype(att_ref.dtype)
    for k in range(steps):
        o_w.pass_y(1, k)
    o_w.finish()
    blocks = depth // width

    def project(j, carry):
        zx = j * width // ow_ref.shape[0]
        per = net.ys * CORES
        w = wo[zx // (net.xs * per), zx // per % net.xs].reshape(per * ow_ref.shape[0], q_width)
        out_ref[:, pl.ds(pl.multiple_of(j * width, width), width)] = lax.dot_general(
            att_ref[...], w, (((1,), (1,)), ((), ())), preferred_element_type=jnp.float32
        ).astype(out_ref.dtype)
        return carry

    lax.fori_loop(0, blocks, project, 0)
    kv_w.drain()
    q_w.drain()
    o_w.drain()
    kv.drain()


def vmem():
    return pl.BlockSpec(memory_space=pltpu.VMEM)


def fast(dims, tokens, q_weight, k_weight, v_weight, out_weight, q_gain, k_gain):
    zs, xs, ys = dims
    rows_in = tokens[0]
    rows, depth = rows_in.shape
    head_width = q_gain.shape[0]
    q_width = out_weight.shape[0]
    kv_width = k_weight.shape[1]
    groups = kv_width // head_width
    group = q_width // kv_width
    pair = 2 * head_width
    own = q_weight.shape[0]
    sums = 16
    dma = pltpu.SemaphoreType.DMA
    bf16, f32 = jnp.bfloat16, jnp.float32
    gather_sems = [
        dma((zs,)), dma((zs,)), dma((zs,)), dma((zs,)),
        dma((2, zs)), dma((2, zs)), dma((4, zs)), dma((4, zs)),
    ]
    grid = (zs, xs, ys, CORES, own)
    out = pl.pallas_call(
        functools.partial(layer_kernel, dims, group, head_width ** (-0.5), head_width),
        out_shape=jax.ShapeDtypeStruct((rows, depth), bf16),
        in_specs=[pl.BlockSpec(memory_space=pl.ANY)] + [vmem()] * 6,
        out_specs=vmem(),
        scratch_shapes=[
            pltpu.VMEM((rows, depth), bf16),
            pltpu.VMEM(grid + (2 * kv_width,), bf16),
            pltpu.VMEM(grid + (q_width,), bf16),
            pltpu.VMEM(grid + (q_width,), bf16),
            pltpu.VMEM((groups, 2 * pair, group * rows), bf16),
            pltpu.VMEM((zs, xs, rows, kv_width), bf16),
            pltpu.VMEM((zs, xs, groups, head_width + sums, rows), bf16),
            pltpu.VMEM((groups, head_width + sums, group * rows), f32),
            pltpu.VMEM((groups, 1, group * rows), f32),
            pltpu.VMEM((rows, q_width), bf16),
            pltpu.VMEM((rows, pair), f32),
            pltpu.VMEM((rows, pair), f32),
            dma,
        ]
        + gather_sems * 3
        + [dma((2, zs)), dma((2, zs)), dma((2, zs)), dma((2, zs))],
        compiler_params=pltpu.CompilerParams(
            collective_id=0, has_side_effects=True, vmem_limit_bytes=VMEM_BYTES
        ),
        cost_estimate=pl.CostEstimate(
            flops=100_000_000_000, bytes_accessed=10_000_000, transcendentals=20_000_000
        ),
    )(
        rows_in, q_weight, k_weight, v_weight, out_weight.T,
        q_gain.reshape(1, head_width), k_gain.reshape(1, head_width),
    )
    return out[None]


def normalize(tensor, gain_vec):
    mean_sq = jnp.mean(tensor * tensor, axis=-1, keepdims=True)
    return tensor * lax.rsqrt(mean_sq + epsilon) * gain_vec


def rotate(tensor, offset):
    row_count = tensor.shape[0]
    head_width = tensor.shape[2]
    quarter = head_width // 4
    half_width = head_width // 2
    positions = jnp.arange(row_count, dtype=jnp.int32) + offset
    frequency = rope_base ** (-jnp.arange(quarter, dtype=jnp.float32) / quarter)

    def rotate_pair(segment, coords):
        angles = coords.astype(jnp.float32)[:, None] * frequency[None, :]
        cosine = jnp.cos(angles)[:, None, :]
        sine_val = jnp.sin(angles)[:, None, :]
        low_half = segment[..., :quarter]
        high_half = segment[..., quarter:]
        return jnp.concatenate(
            [low_half * cosine - high_half * sine_val, high_half * cosine + low_half * sine_val],
            axis=-1,
        )

    return jnp.concatenate(
        [
            rotate_pair(tensor[..., :half_width], positions // GRID_W),
            rotate_pair(tensor[..., half_width:], positions % GRID_W),
        ],
        axis=-1,
    )


def attend(query_rows, key_rows, value_rows):
    row_count, head_width = query_rows.shape
    block_rows = math.gcd(row_count, 512)
    score_scale = head_width ** (-0.5)

    def attend_block(segment):
        scores = (
            lax.dot_general(
                segment, key_rows, (((1,), (1,)), ((), ())), preferred_element_type=jnp.float32
            )
            * score_scale
        )
        row_max = jnp.max(scores, axis=-1, keepdims=True)
        weights = jnp.exp(scores - row_max)
        shares = (weights / jnp.sum(weights, axis=-1, keepdims=True)).astype(jnp.bfloat16)
        return jnp.dot(shares, value_rows, preferred_element_type=jnp.float32).astype(jnp.bfloat16)

    blocks = query_rows.reshape(row_count // block_rows, block_rows, head_width)
    return lax.map(attend_block, blocks).reshape(row_count, head_width)


def plain(tokens, q_weight, k_weight, v_weight, out_weight, q_gain, k_gain):
    rows_in = tokens[0]
    tok_count = rows_in.shape[0]
    head_width = q_gain.shape[0]
    q_width = out_weight.shape[0]
    kv_width = k_weight.shape[1]
    q_heads = q_width // head_width
    kv_heads = kv_width // head_width
    group_size = q_heads // kv_heads
    sp_count = lax.axis_size("sp")
    offset = lax.axis_index("sp") * tok_count
    weight_rows = (
        lax.all_gather(q_weight, ("sp", "dp"), axis=0, tiled=True),
        lax.all_gather(k_weight, ("sp", "dp"), axis=0, tiled=True),
        lax.all_gather(v_weight, ("sp", "dp"), axis=0, tiled=True),
    )
    query_raw, key_raw, value_raw = tuple(
        (
            jnp.dot(rows_in, rows_part, preferred_element_type=jnp.float32)
            for rows_part in weight_rows
        )
    )
    queries = rotate(
        normalize(query_raw.reshape(tok_count, q_heads, head_width), q_gain), offset
    ).astype(jnp.bfloat16)
    keys_rot = rotate(
        normalize(key_raw.reshape(tok_count, kv_heads, head_width), k_gain), offset
    ).astype(jnp.bfloat16)
    values_dev = value_raw.astype(jnp.bfloat16)
    keys_wide = jnp.broadcast_to(
        keys_rot[:, :, None, :], (tok_count, kv_heads, group_size, head_width)
    ).reshape(tok_count, q_width)
    values_wide = jnp.broadcast_to(
        values_dev.reshape(tok_count, kv_heads, 1, head_width),
        (tok_count, kv_heads, group_size, head_width),
    ).reshape(tok_count, q_width)
    q_local, k_local, v_local = (
        lax.all_to_all(
            queries.reshape(tok_count, q_width), "sp", split_axis=1, concat_axis=0, tiled=True
        ),
        lax.all_to_all(keys_wide, "sp", split_axis=1, concat_axis=0, tiled=True),
        lax.all_to_all(values_wide, "sp", split_axis=1, concat_axis=0, tiled=True),
    )
    local_heads = q_width // sp_count // head_width
    outputs = []
    for head_index in range(local_heads):
        low_col = head_index * head_width
        outputs.append(
            attend(
                q_local[:, low_col : low_col + head_width],
                k_local[:, low_col : low_col + head_width],
                v_local[:, low_col : low_col + head_width],
            )
        )
    head_results = jnp.concatenate(outputs, axis=1)
    attended = lax.all_to_all(head_results, "sp", split_axis=0, concat_axis=1, tiled=True)
    result = jnp.dot(
        attended,
        lax.all_gather(out_weight, ("sp", "dp"), axis=1, tiled=True),
        preferred_element_type=jnp.float32,
    ).astype(jnp.bfloat16)
    return result[None]


def solution(mesh):
    sp, dp = mesh.shape["sp"], mesh.shape["dp"]
    across = dp // CORES
    exchange = dp == 2 * CORES and sp % across == 0 and sp // across > 1
    body = functools.partial(fast, (sp // across, across, across)) if exchange else plain
    return jax.shard_map(
        body,
        mesh=mesh,
        in_specs=(
            P("dp", "sp", None),
            P(("sp", "dp"), None),
            P(("sp", "dp"), None),
            P(("sp", "dp"), None),
            P(None, ("sp", "dp")),
            P(),
            P(),
        ),
        out_specs=P("dp", "sp", None),
        check_vma=False,
    )
```

```python
import functools
import math

import jax
import jax.numpy as jnp
from jax import lax
from jax.experimental import pallas as pl
from jax.experimental.pallas import tpu as pltpu
from jax.sharding import PartitionSpec as P

GRID_W = 64
CORES = 2
epsilon = 1e-06
rope_base = 10000.0
VMEM_BYTES = 60 * 1024 * 1024


class Net:
    def __init__(self, dims):
        self.zs, self.xs, self.ys = dims
        sp, dp = lax.axis_index("sp"), lax.axis_index("dp")
        self.z, self.x = sp // self.xs, sp % self.xs
        self.y, self.c = dp // CORES, dp % CORES
        self.ox, self.oy, self.oc = 1 - self.x, 1 - self.y, 1 - self.c

    def at(self, z=None, x=None, y=None, c=None):
        z = self.z if z is None else z
        x = self.x if x is None else x
        y = self.y if y is None else y
        c = self.c if c is None else c
        return {"sp": z * self.xs + x, "dp": y * CORES + c}

    def inside(self, z):
        return jnp.logical_and(z >= 0, z < self.zs)

    def near(self, k):
        below, above = self.z, self.zs - 1 - self.z
        both = jnp.minimum(below, above)
        inner = k <= 2 * both
        far = jnp.where(above > below, 1, -1)
        sign = jnp.where(inner, jnp.where(k % 2 == 1, 1, -1), far)
        return self.z + sign * jnp.where(inner, (k + 1) // 2, k - both)


def remote(src, dst, send, recv, where):
    return pltpu.make_async_remote_copy(
        src_ref=src,
        dst_ref=dst,
        send_sem=send,
        recv_sem=recv,
        device_id=where,
        device_id_type=pl.DeviceIdType.MESH,
    )


class Gather:
    def __init__(self, net, buf, split, sems):
        self.net, self.buf, self.split = net, buf, split
        self.zs, self.zr, self.xs, self.xr, self.ys, self.yr, self.cs, self.cr = sems

    def block(self, k, kind, c=None):
        net = self.net
        x = net.ox if kind % 2 else net.x
        y = net.oy if kind // 2 else net.y
        return self.buf.at[net.near(k), x, y, net.c if c is None else c]

    def half(self, k, kind, h):
        net, wide = self.net, self.buf.shape[-1] // 2
        x = net.ox if kind % 2 else net.x
        y = net.oy if kind // 2 else net.y
        return self.buf.at[net.near(k), x, y, net.c, :, pl.ds(h * wide, wide)]

    def over_z(self, k):
        net, b = self.net, self.block(0, 0)
        return remote(b, b, self.zs.at[k - 1], self.zr.at[net.z], net.at(z=net.near(k)))

    def from_z(self, k):
        net, b = self.net, self.block(k, 0)
        return remote(b, b, self.zs.at[k - 1], self.zr.at[net.near(k)], net.at(z=net.near(k)))

    def over_x(self, k, arriving=False):
        b = self.block(k, 1 if arriving else 0)
        return remote(b, b, self.xs.at[0, k], self.xr.at[0, k], self.net.at(x=self.net.ox))

    def half_x(self, k, arriving=False):
        b = self.half(k, 3 if arriving else 2, 1)
        return remote(b, b, self.xs.at[1, k], self.xr.at[1, k], self.net.at(x=self.net.ox))

    def over_y(self, k, arriving=False):
        b = self.block(k, 2 if arriving else 0)
        return remote(b, b, self.ys.at[0, k], self.yr.at[0, k], self.net.at(y=self.net.oy))

    def corner_y(self, k, arriving=False):
        kind = 3 if arriving else 1
        b = self.half(k, kind, 0) if self.split else self.block(k, kind)
        return remote(b, b, self.ys.at[1, k], self.yr.at[1, k], self.net.at(y=self.net.oy))

    def over_c(self, kind, k, arriving=False):
        b = self.block(k, kind, self.net.oc if arriving else None)
        return remote(b, b, self.cs.at[kind, k], self.cr.at[kind, k], self.net.at(c=self.net.oc))

    def start_z(self):
        for k in reversed(range(1, self.net.zs)):
            self.over_z(k).start()

    def spread(self, k):
        self.over_y(k).start()
        self.over_x(k).start()
        self.over_c(0, k).start()

    def pass_z(self, k):
        self.from_z(k).wait_recv()
        self.spread(k)

    def pass_x(self, k):
        self.over_x(k, True).wait_recv()
        self.corner_y(k).start()
        self.over_c(1, k).start()

    def pass_y(self, k):
        self.over_y(k, True).wait_recv()
        if self.split:
            self.half_x(k).start()
        self.over_c(2, k).start()

    def pass_corner(self, k):
        self.corner_y(k, True).wait_recv()
        if self.split:
            self.half_x(k, True).wait_recv()
        self.over_c(3, k).start()

    def finish(self):
        for k in range(self.net.zs):
            for kind in range(4):
                self.over_c(kind, k, True).wait_recv()

    def drain(self):
        for k in range(self.net.zs):
            if k:
                self.over_z(k).wait_send()
            self.over_x(k).wait_send()
            self.over_y(k).wait_send()
            self.corner_y(k).wait_send()
            if self.split:
                self.half_x(k).wait_send()
            for kind in range(4):
                self.over_c(kind, k).wait_send()


class Chain:
    def __init__(self, net, send, recv):
        self.net, self.send, self.recv = net, send, recv

    def own(self, side):
        net = self.net
        to = net.z + (1 if side else -1)
        b = self.part(net.z)
        return to, remote(
            b, b, self.send.at[net.zs * side], self.recv.at[net.z], net.at(z=to)
        )

    def arrival(self, k):
        z = self.net.near(k)
        b = self.part(z)
        return remote(b, b, self.send.at[k], self.recv.at[z], self.net.at(z=z))

    def onward(self, k):
        net = self.net
        z = net.near(k)
        to = net.z + jnp.where(z > net.z, -1, 1)
        b = self.part(z)
        return to, remote(b, b, self.send.at[k], self.recv.at[z], net.at(z=to))

    def each(self, one, act):
        to, copy = one

        @pl.when(self.net.inside(to))
        def _():
            act(copy)

    def start(self):
        for side in range(2):
            self.each(self.own(side), lambda copy: copy.start())

    def receive(self, k):
        self.arrival(k).wait_recv()
        self.each(self.onward(k), lambda copy: copy.start())

    def drain(self):
        for side in range(2):
            self.each(self.own(side), lambda copy: copy.wait_send())
        for k in range(1, self.net.zs):
            self.each(self.onward(k), lambda copy: copy.wait_send())


class KeyChain(Chain):
    def __init__(self, net, buf, own, rows, sems):
        super().__init__(net, sems[0], sems[1])
        self.buf, self.mine, self.rows = buf, own, rows
        self.cs, self.cr, self.ss, self.sr = sems[2:]

    def part(self, z, c=None):
        c = self.net.c if c is None else c
        if self.rows is None:
            return self.buf.at[z, c]
        return self.buf.at[z, c, :, : self.rows]

    def swap(self, arriving=False):
        net = self.net
        dst = self.part(net.z, None if arriving else net.x)
        return remote(self.mine, dst, self.ss, self.sr, net.at(x=net.ox, c=net.oc))

    def over_c(self, k, arriving=False):
        net = self.net
        b = self.part(net.near(k), net.oc if arriving else None)
        return remote(b, b, self.cs.at[k], self.cr.at[k], net.at(c=net.oc))

    def begin(self):
        self.start()
        self.over_c(0).start()

    def pass_swap(self):
        self.swap(True).wait_recv()
        self.begin()

    def pass_z(self, k):
        self.receive(k)
        self.over_c(k).start()

    def arrived(self, k):
        self.over_c(k, True).wait_recv()

    def drain(self):
        super().drain()
        for k in range(self.net.zs):
            self.over_c(k).wait_send()


def greet(net):
    barrier = pltpu.get_barrier_semaphore()
    others = [net.at(x=net.ox), net.at(y=net.oy), net.at(c=net.oc)]
    others += [net.at(x=net.ox, c=net.oc)]
    others += [net.at(z=net.near(k)) for k in range(1, net.zs)]
    for where in others:
        pl.semaphore_signal(barrier, inc=1, device_id=where, device_id_type=pl.DeviceIdType.MESH)
    pl.semaphore_wait(barrier, len(others))


def layer_kernel(
    dims, group, scale, head_width, tok_hbm, qw_ref, kw_ref, vw_ref, ow_ref, qg_ref, kg_ref,
    out_ref, tok_ref, wkv, wq0, wq1, wo, q_ref, k_buf, v_buf, acc_ref, max_ref, att_ref,
    k_own, v_own, q_own, q_in, att_own, cos_ref, sin_ref, tok_sem, *sems
):
    net = Net(dims)
    rows, depth = tok_ref.shape
    pair = 2 * head_width
    kv_width = kw_ref.shape[1]
    groups = kv_width // head_width
    q_width = qw_ref.shape[1]
    width = 4 * head_width
    load = pltpu.make_async_copy(tok_hbm, tok_ref, tok_sem)
    load.start()
    me = (net.z, net.x, net.y, net.c)
    wkv[me + (slice(None), slice(0, kv_width))] = kw_ref[...]
    wkv[me + (slice(None), slice(kv_width, 2 * kv_width))] = vw_ref[...]
    half = q_width // 2
    wq0[me] = qw_ref[:, :half]
    wq1[me] = qw_ref[:, half:]
    wo[me] = ow_ref[...]
    kv_w = Gather(net, wkv, True, sems[0:8])
    q_w = [Gather(net, buf, False, sems[8 * i : 8 * i + 8]) for i, buf in ((1, wq0), (2, wq1))]
    o_w = Gather(net, wo, False, sems[24:32])
    keys = KeyChain(net, k_buf, k_own, None, sems[32:38])
    values = KeyChain(net, v_buf, v_own, head_width, sems[38:44])
    q_send, q_recv, a_send, a_recv = sems[44:]
    native = net.c == net.x
    foreign = net.c != net.x
    steps = net.zs
    greet(net)
    kv_w.start_z()
    kv_w.spread(0)

    lane = lax.broadcasted_iota(jnp.int32, (rows, pair), 1)
    at = lax.broadcasted_iota(jnp.int32, (rows, pair), 0) + (net.z * net.xs + net.x) * rows
    quarter = head_width // 4
    power = (lane % quarter).astype(jnp.float32) * (-math.log(rope_base) / quarter)
    spot = jnp.where(lane % head_width < 2 * quarter, at // GRID_W, at % GRID_W)
    angle = spot.astype(jnp.float32) * jnp.exp(power)
    first = lane % (2 * quarter) < quarter
    cos_ref[...] = jnp.cos(angle)
    sin_ref[...] = jnp.where(first, -jnp.sin(angle), jnp.sin(angle))

    q_ref[...] = jnp.zeros_like(q_ref)
    acc_ref[...] = jnp.zeros_like(acc_ref)
    max_ref[...] = jnp.full_like(max_ref, -jnp.inf)
    tail = v_buf.shape[3] - head_width
    v_buf[:, :, :, head_width:] = jnp.ones(v_buf.shape[:3] + (tail, rows), v_buf.dtype)
    load.wait()

    r = lax.broadcasted_iota(jnp.int32, (2 * width, width), 0) % width // head_width
    c = lax.broadcasted_iota(jnp.int32, (2 * width, width), 1) // head_width
    averager = jnp.where(r == c, 1.0 / head_width, 0.0).astype(jnp.bfloat16)
    wide_first = jnp.concatenate([first, first], axis=1)

    def twice(ref):
        return jnp.concatenate([ref[...]] * 2, axis=1)

    def product(buf, at):
        w = buf[:, :, :, :, :, at : at + width].reshape(depth, width)
        return jnp.dot(tok_ref[...], w, preferred_element_type=jnp.float32)

    def halves(t):
        high = t.astype(jnp.bfloat16)
        return high, (t - high.astype(jnp.float32)).astype(jnp.bfloat16)

    def turned(t, gain_ref):
        gain = jnp.concatenate([gain_ref[...]] * 4, axis=1)
        mean_sq = jnp.dot(
            jnp.concatenate(halves(t * t), axis=1), averager, preferred_element_type=jnp.float32
        )
        t = t * lax.rsqrt(mean_sq + epsilon) * gain
        other = jnp.where(
            wide_first, pltpu.roll(t, width - quarter, 1), pltpu.roll(t, quarter, 1)
        )
        return t * twice(cos_ref) + other * twice(sin_ref)

    for k in range(1, steps):
        kv_w.pass_z(k)
    q_w[0].start_z()
    for k in range(steps):
        kv_w.pass_x(k)
        kv_w.pass_y(k)
    q_w[0].spread(0)
    q_w[1].start_z()
    for k in range(steps):
        kv_w.pass_corner(k)
    for k in range(1, steps):
        q_w[0].pass_z(k)
    q_w[0].pass_x(0)
    kv_w.finish()
    k_own[...] = turned(product(wkv, 0), kg_ref).astype(k_buf.dtype)
    v_own[...] = product(wkv, kv_width).T.astype(v_buf.dtype).reshape(v_own.shape)

    @pl.when(native)
    def _():
        k_buf[net.z, net.c] = k_own[...]
        v_buf[net.z, net.c, :, :head_width] = v_own[...]
        keys.begin()
        values.begin()

    @pl.when(foreign)
    def _():
        keys.swap().start()
        values.swap().start()

    for k in range(1, steps):
        q_w[0].pass_x(k)
    q_w[1].spread(0)
    for k in range(1, steps):
        q_w[1].pass_z(k)
    for k in range(steps):
        q_w[0].pass_y(k)

    @pl.when(foreign)
    def _():
        keys.pass_swap()
        values.pass_swap()

    for k in range(steps):
        q_w[0].pass_corner(k)
    for k in range(steps):
        q_w[1].pass_x(k)
    q_w[0].finish()

    def both(act, k):
        getattr(keys, act)(k)
        getattr(values, act)(k)

    edge = jnp.logical_or(net.z == 0, net.z == net.zs - 1)

    def early(act, inside, *where):
        @pl.when(edge != inside)
        def _():
            act(*where)

    def q_swap(g):
        return remote(
            q_own.at[g], q_in.at[g], q_send.at[g], q_recv.at[g], net.at(x=net.ox, c=net.oc)
        )

    def a_swap(g):
        return remote(
            att_own.at[g], att_ref.at[g], a_send.at[g], a_recv.at[g], net.at(x=net.ox, c=net.oc)
        )

    def project_queries(g):
        w = (wq0, wq1)[g * width // half]
        q = turned(product(w, g * width % half), qg_ref).astype(jnp.bfloat16)

        @pl.when(native)
        def _():
            q_in[g] = q

        @pl.when(foreign)
        def _():
            q_own[g] = q
            q_swap(g).start()

    def place_queries(g):
        @pl.when(foreign)
        def _():
            q_swap(g).wait_recv()

        q = (q_in[g].astype(jnp.float32) * (scale * math.log2(math.e))).T
        base = (g % 2) * head_width
        for i, part in enumerate(halves(q)):
            for n in range(group):
                q_ref[
                    g, i * pair + base : i * pair + base + head_width, n * rows : (n + 1) * rows
                ] = part[n * head_width : (n + 1) * head_width]

    def later_queries():
        for k in range(steps):
            q_w[1].pass_y(k)
        for k in range(steps):
            q_w[1].pass_corner(k)
        q_w[1].finish()
        for g in range(groups // 2, groups):
            project_queries(g)

    def place_later():
        for g in range(groups // 2, groups):
            place_queries(g)

    for g in range(groups // 2):
        project_queries(g)

    chunk = width
    keys_now = net.xs * rows
    chunks = group * rows // chunk

    def attend(k, g):
        z = net.near(k)
        k_now = k_buf[z, :, :, pl.ds(pl.multiple_of(g // 2 * pair, pair), pair)]
        k_now = k_now.reshape(keys_now, pair)
        k_now = jnp.concatenate([k_now, k_now], axis=1)
        v_now = jnp.concatenate([v_buf[z, x, g] for x in range(net.xs)], axis=1)
        cols = [slice(n * chunk, (n + 1) * chunk) for n in range(chunks)]
        scores = [
            jnp.dot(k_now, q_ref[g, :, at], preferred_element_type=jnp.float32) for at in cols
        ]
        for at, s in zip(cols, scores):
            old = max_ref[g, :, at]
            top = jnp.maximum(old, jnp.max(s, axis=0, keepdims=True))
            p = jnp.exp2(s - top).astype(v_now.dtype)
            max_ref[g, :, at] = top
            acc_ref[g, :, at] = acc_ref[g, :, at] * jnp.exp2(old - top) + jnp.dot(
                v_now, p, preferred_element_type=jnp.float32
            )

    events = {t: [] for t in range(steps * groups)}
    both("pass_z", 1)
    early(both, True, "pass_z", 2)
    o_w.start_z()
    o_w.spread(0)
    for g in range(groups // 2):
        place_queries(g)
    both("arrived", 0)
    events[2].append((both, "arrived", 1))
    events[2].append((later_queries,))
    events[4].append((place_later,))
    events[4].append((early, both, True, "pass_z", 3))
    events[4].append((early, both, False, "pass_z", 2))
    events[8].append((early, both, False, "pass_z", 3))
    for k in range(2, steps):
        events[k * groups].append((both, "arrived", k))
    for k in range(1, steps):
        events[groups + 1].append((o_w.pass_z, k))
    for k in range(steps):
        events[2 * groups].append((o_w.pass_x, k))
        events[2 * groups].append((o_w.pass_y, k))
        events[3 * groups + k].append((o_w.pass_corner, k))

    def settle(g):
        parts = []
        for n in range(group):
            cols = slice(n * rows, (n + 1) * rows)
            total = acc_ref[g, head_width : head_width + 1, cols]
            parts.append(acc_ref[g, :head_width, cols] / total)
        a = jnp.concatenate(parts, axis=0).T.astype(att_ref.dtype)

        @pl.when(native)
        def _():
            att_ref[g] = a

        @pl.when(foreign)
        def _():
            att_own[g] = a
            a_swap(g).start()

    def step(t, carry):
        head = t < 2 * groups
        k = jnp.where(head, t % groups // 2, t // groups)
        g = jnp.where(head, t // groups * 2 + t % 2, t % groups)
        for when, todo in events.items():
            if todo:

                @pl.when(t == when)
                def _():
                    for act, *where in todo:
                        act(*where)

        attend(k, g)

        @pl.when(k == steps - 1)
        def _():
            settle(g)

        return carry

    lax.fori_loop(0, steps * groups, step, 0)

    o_w.finish()
    across = 2 * width

    @pl.when(foreign)
    def _():
        for g in range(groups):
            a_swap(g).wait_recv()

    attended = jnp.concatenate([att_ref[g] for g in range(groups)], axis=1)

    def project(j, carry):
        w = wo[j].reshape(across, q_width)
        out_ref[:, pl.ds(pl.multiple_of(j * across, across), across)] = lax.dot_general(
            attended, w, (((1,), (1,)), ((), ())), preferred_element_type=jnp.float32
        ).astype(out_ref.dtype)
        return carry

    lax.fori_loop(0, depth // across, project, 0)
    for part in (kv_w, *q_w, o_w, keys, values):
        part.drain()

    @pl.when(foreign)
    def _():
        keys.swap().wait_send()
        values.swap().wait_send()
        for g in range(groups):
            q_swap(g).wait_send()
            a_swap(g).wait_send()


def vmem():
    return pl.BlockSpec(memory_space=pltpu.VMEM)


def fast(dims, tokens, q_weight, k_weight, v_weight, out_weight, q_gain, k_gain):
    zs, xs, ys = dims
    rows_in = tokens[0]
    rows, depth = rows_in.shape
    head_width = q_gain.shape[0]
    q_width = out_weight.shape[0]
    kv_width = k_weight.shape[1]
    groups = kv_width // head_width
    group = q_width // kv_width
    pair = 2 * head_width
    own = q_weight.shape[0]
    sums = 16
    dma = pltpu.SemaphoreType.DMA
    bf16, f32 = jnp.bfloat16, jnp.float32
    gather_sems = [
        dma((zs,)), dma((zs,)), dma((2, zs)), dma((2, zs)),
        dma((2, zs)), dma((2, zs)), dma((4, zs)), dma((4, zs)),
    ]
    key_sems = [dma((zs + 1,)), dma((zs,)), dma((zs,)), dma((zs,)), dma, dma]
    grid = (zs, xs, ys, CORES, own)
    out = pl.pallas_call(
        functools.partial(layer_kernel, dims, group, head_width ** (-0.5), head_width),
        out_shape=pltpu.VMEM((rows, depth), bf16),
        in_specs=[pl.BlockSpec(memory_space=pl.ANY)] + [vmem()] * 6,
        out_specs=vmem(),
        scratch_shapes=[
            pltpu.VMEM((rows, depth), bf16),
            pltpu.VMEM(grid + (2 * kv_width,), bf16),
            pltpu.VMEM(grid + (q_width // 2,), bf16),
            pltpu.VMEM(grid + (q_width // 2,), bf16),
            pltpu.VMEM(grid + (q_width,), bf16),
            pltpu.VMEM((groups, 2 * pair, group * rows), bf16),
            pltpu.VMEM((zs, xs, rows, kv_width), bf16),
            pltpu.VMEM((zs, xs, groups, head_width + sums, rows), bf16),
            pltpu.VMEM((groups, head_width + sums, group * rows), f32),
            pltpu.VMEM((groups, 1, group * rows), f32),
            pltpu.VMEM((groups, rows, group * head_width), bf16),
            pltpu.VMEM((rows, kv_width), bf16),
            pltpu.VMEM((groups, head_width, rows), bf16),
            pltpu.VMEM((groups, rows, group * head_width), bf16),
            pltpu.VMEM((groups, rows, group * head_width), bf16),
            pltpu.VMEM((groups, rows, group * head_width), bf16),
            pltpu.VMEM((rows, pair), f32),
            pltpu.VMEM((rows, pair), f32),
            dma,
        ]
        + gather_sems * 4
        + key_sems * 2
        + [dma((groups,))] * 4,
        compiler_params=pltpu.CompilerParams(
            collective_id=0, has_side_effects=True, vmem_limit_bytes=VMEM_BYTES
        ),
        cost_estimate=pl.CostEstimate(
            flops=100_000_000_000, bytes_accessed=10_000_000, transcendentals=20_000_000
        ),
    )(
        rows_in, q_weight, k_weight, v_weight, out_weight.T,
        q_gain.reshape(1, head_width), k_gain.reshape(1, head_width),
    )
    return out[None]


def normalize(tensor, gain_vec):
    mean_sq = jnp.mean(tensor * tensor, axis=-1, keepdims=True)
    return tensor * lax.rsqrt(mean_sq + epsilon) * gain_vec


def rotate(tensor, offset):
    row_count = tensor.shape[0]
    head_width = tensor.shape[2]
    quarter = head_width // 4
    half_width = head_width // 2
    positions = jnp.arange(row_count, dtype=jnp.int32) + offset
    frequency = rope_base ** (-jnp.arange(quarter, dtype=jnp.float32) / quarter)

    def rotate_pair(segment, coords):
        angles = coords.astype(jnp.float32)[:, None] * frequency[None, :]
        cosine = jnp.cos(angles)[:, None, :]
        sine_val = jnp.sin(angles)[:, None, :]
        low_half = segment[..., :quarter]
        high_half = segment[..., quarter:]
        return jnp.concatenate(
            [low_half * cosine - high_half * sine_val, high_half * cosine + low_half * sine_val],
            axis=-1,
        )

    return jnp.concatenate(
        [
            rotate_pair(tensor[..., :half_width], positions // GRID_W),
            rotate_pair(tensor[..., half_width:], positions % GRID_W),
        ],
        axis=-1,
    )


def attend(query_rows, key_rows, value_rows):
    row_count, head_width = query_rows.shape
    block_rows = math.gcd(row_count, 512)
    score_scale = head_width ** (-0.5)

    def attend_block(segment):
        scores = (
            lax.dot_general(
                segment, key_rows, (((1,), (1,)), ((), ())), preferred_element_type=jnp.float32
            )
            * score_scale
        )
        row_max = jnp.max(scores, axis=-1, keepdims=True)
        weights = jnp.exp(scores - row_max)
        shares = (weights / jnp.sum(weights, axis=-1, keepdims=True)).astype(jnp.bfloat16)
        return jnp.dot(shares, value_rows, preferred_element_type=jnp.float32).astype(jnp.bfloat16)

    blocks = query_rows.reshape(row_count // block_rows, block_rows, head_width)
    return lax.map(attend_block, blocks).reshape(row_count, head_width)


def plain(tokens, q_weight, k_weight, v_weight, out_weight, q_gain, k_gain):
    rows_in = tokens[0]
    tok_count = rows_in.shape[0]
    head_width = q_gain.shape[0]
    q_width = out_weight.shape[0]
    kv_width = k_weight.shape[1]
    q_heads = q_width // head_width
    kv_heads = kv_width // head_width
    group_size = q_heads // kv_heads
    sp_count = lax.axis_size("sp")
    offset = lax.axis_index("sp") * tok_count
    weight_rows = (
        lax.all_gather(q_weight, ("sp", "dp"), axis=0, tiled=True),
        lax.all_gather(k_weight, ("sp", "dp"), axis=0, tiled=True),
        lax.all_gather(v_weight, ("sp", "dp"), axis=0, tiled=True),
    )
    query_raw, key_raw, value_raw = tuple(
        (
            jnp.dot(rows_in, rows_part, preferred_element_type=jnp.float32)
            for rows_part in weight_rows
        )
    )
    queries = rotate(
        normalize(query_raw.reshape(tok_count, q_heads, head_width), q_gain), offset
    ).astype(jnp.bfloat16)
    keys_rot = rotate(
        normalize(key_raw.reshape(tok_count, kv_heads, head_width), k_gain), offset
    ).astype(jnp.bfloat16)
    values_dev = value_raw.astype(jnp.bfloat16)
    keys_wide = jnp.broadcast_to(
        keys_rot[:, :, None, :], (tok_count, kv_heads, group_size, head_width)
    ).reshape(tok_count, q_width)
    values_wide = jnp.broadcast_to(
        values_dev.reshape(tok_count, kv_heads, 1, head_width),
        (tok_count, kv_heads, group_size, head_width),
    ).reshape(tok_count, q_width)
    q_local, k_local, v_local = (
        lax.all_to_all(
            queries.reshape(tok_count, q_width), "sp", split_axis=1, concat_axis=0, tiled=True
        ),
        lax.all_to_all(keys_wide, "sp", split_axis=1, concat_axis=0, tiled=True),
        lax.all_to_all(values_wide, "sp", split_axis=1, concat_axis=0, tiled=True),
    )
    local_heads = q_width // sp_count // head_width
    outputs = []
    for head_index in range(local_heads):
        low_col = head_index * head_width
        outputs.append(
            attend(
                q_local[:, low_col : low_col + head_width],
                k_local[:, low_col : low_col + head_width],
                v_local[:, low_col : low_col + head_width],
            )
        )
    head_results = jnp.concatenate(outputs, axis=1)
    attended = lax.all_to_all(head_results, "sp", split_axis=0, concat_axis=1, tiled=True)
    result = jnp.dot(
        attended,
        lax.all_gather(out_weight, ("sp", "dp"), axis=1, tiled=True),
        preferred_element_type=jnp.float32,
    ).astype(jnp.bfloat16)
    return result[None]


def solution(mesh):
    sp, dp = mesh.shape["sp"], mesh.shape["dp"]
    across = dp // CORES
    exchange = dp == 2 * CORES and sp % across == 0 and sp // across > 1
    body = functools.partial(fast, (sp // across, across, across)) if exchange else plain
    return jax.shard_map(
        body,
        mesh=mesh,
        in_specs=(
            P("dp", "sp", None),
            P(("sp", "dp"), None),
            P(("sp", "dp"), None),
            P(("sp", "dp"), None),
            P(None, ("sp", "dp")),
            P(),
            P(),
        ),
        out_specs=P("dp", "sp", None),
        check_vma=False,
    )
```

```python
import functools
import math

import jax
import jax.numpy as jnp
from jax import lax
from jax.experimental import pallas as pl
from jax.experimental.pallas import tpu as pltpu
from jax.sharding import PartitionSpec as P

GRID_W = 64
CORES = 2
epsilon = 1e-06
rope_base = 10000.0
VMEM_BYTES = 60 * 1024 * 1024


class Net:
    def __init__(self, dims):
        self.zs, self.xs, self.ys = dims
        sp, dp = lax.axis_index("sp"), lax.axis_index("dp")
        self.z, self.x = sp // self.xs, sp % self.xs
        self.y, self.c = dp // CORES, dp % CORES
        self.ox, self.oy, self.oc = 1 - self.x, 1 - self.y, 1 - self.c

    def at(self, z=None, x=None, y=None, c=None):
        z = self.z if z is None else z
        x = self.x if x is None else x
        y = self.y if y is None else y
        c = self.c if c is None else c
        return {"sp": z * self.xs + x, "dp": y * CORES + c}

    def inside(self, z):
        return jnp.logical_and(z >= 0, z < self.zs)

    def near(self, k):
        below, above = self.z, self.zs - 1 - self.z
        both = jnp.minimum(below, above)
        inner = k <= 2 * both
        far = jnp.where(above > below, 1, -1)
        sign = jnp.where(inner, jnp.where(k % 2 == 1, 1, -1), far)
        return self.z + sign * jnp.where(inner, (k + 1) // 2, k - both)


def remote(src, dst, send, recv, where):
    return pltpu.make_async_remote_copy(
        src_ref=src,
        dst_ref=dst,
        send_sem=send,
        recv_sem=recv,
        device_id=where,
        device_id_type=pl.DeviceIdType.MESH,
    )


class Gather:
    def __init__(self, net, buf, split, sems):
        self.net, self.buf, self.split = net, buf, split
        self.zs, self.zr, self.xs, self.xr, self.ys, self.yr, self.cs, self.cr = sems

    def block(self, k, kind, c=None):
        net = self.net
        x = net.ox if kind % 2 else net.x
        y = net.oy if kind // 2 else net.y
        return self.buf.at[net.near(k), x, y, net.c if c is None else c]

    def half(self, k, kind, h):
        net, wide = self.net, self.buf.shape[-1] // 2
        x = net.ox if kind % 2 else net.x
        y = net.oy if kind // 2 else net.y
        return self.buf.at[net.near(k), x, y, net.c, :, pl.ds(h * wide, wide)]

    def over_z(self, k):
        net, b = self.net, self.block(0, 0)
        return remote(b, b, self.zs, self.zr.at[net.z], net.at(z=net.near(k)))

    def from_z(self, k):
        net, b = self.net, self.block(k, 0)
        return remote(b, b, self.zs, self.zr.at[net.near(k)], net.at(z=net.near(k)))

    def over_x(self, k, arriving=False):
        b = self.block(k, 1 if arriving else 0)
        return remote(b, b, self.xs, self.xr.at[0, k], self.net.at(x=self.net.ox))

    def half_x(self, k, arriving=False):
        b = self.half(k, 3 if arriving else 2, 1)
        return remote(b, b, self.xs, self.xr.at[1, k], self.net.at(x=self.net.ox))

    def over_y(self, k, arriving=False):
        b = self.block(k, 2 if arriving else 0)
        return remote(b, b, self.ys, self.yr.at[0, k], self.net.at(y=self.net.oy))

    def corner_y(self, k, arriving=False):
        kind = 3 if arriving else 1
        b = self.half(k, kind, 0) if self.split else self.block(k, kind)
        return remote(b, b, self.ys, self.yr.at[1, k], self.net.at(y=self.net.oy))

    def over_c(self, kind, k):
        b = self.block(k, kind)
        return remote(b, b, self.cs, self.cr, self.net.at(c=self.net.oc))

    def bulk(self, sem, steps, xs=1, ys=1, wide=None):
        b = self.buf.at[:steps, :xs, :ys, 0, :, :wide]
        return remote(b, b, sem, self.cr, self.net.at(c=self.net.oc))

    def start_z(self):
        for k in reversed(range(1, self.net.zs)):
            self.over_z(k).start()

    def spread(self, k):
        self.over_y(k).start()
        self.over_x(k).start()
        self.over_c(0, k).start()

    def pass_z(self, k):
        self.from_z(k).wait_recv()
        self.spread(k)

    def pass_x(self, k):
        self.over_x(k, True).wait_recv()
        self.corner_y(k).start()
        self.over_c(1, k).start()

    def pass_y(self, k):
        self.over_y(k, True).wait_recv()
        if self.split:
            self.half_x(k).start()
        self.over_c(2, k).start()

    def pass_corner(self, k):
        self.corner_y(k, True).wait_recv()
        if self.split:
            self.half_x(k, True).wait_recv()
        self.over_c(3, k).start()

    def finish(self):
        self.bulk(self.cs, self.net.zs, self.net.xs, self.net.ys).wait_recv()

    def drain(self):
        net = self.net
        self.bulk(self.zs, net.zs - 1).wait_send()
        self.bulk(self.cs, net.zs, net.xs, net.ys).wait_send()
        if self.split:
            three = 3 * self.buf.shape[-1] // 4
            self.bulk(self.xs, net.zs, net.xs, 1, three).wait_send()
            self.bulk(self.ys, net.zs, 1, net.ys, three).wait_send()
        else:
            self.bulk(self.xs, net.zs).wait_send()
            self.bulk(self.ys, net.zs, 1, net.ys).wait_send()


class Chain:
    def __init__(self, net, send, recv):
        self.net, self.send, self.recv = net, send, recv

    def own(self, side):
        net = self.net
        to = net.z + (1 if side else -1)
        b = self.part(net.z)
        return to, remote(
            b, b, self.send.at[net.zs * side], self.recv.at[net.z], net.at(z=to)
        )

    def arrival(self, k):
        z = self.net.near(k)
        b = self.part(z)
        return remote(b, b, self.send.at[k], self.recv.at[z], self.net.at(z=z))

    def onward(self, k):
        net = self.net
        z = net.near(k)
        to = net.z + jnp.where(z > net.z, -1, 1)
        b = self.part(z)
        return to, remote(b, b, self.send.at[k], self.recv.at[z], net.at(z=to))

    def each(self, one, act):
        to, copy = one

        @pl.when(self.net.inside(to))
        def _():
            act(copy)

    def start(self):
        for side in range(2):
            self.each(self.own(side), lambda copy: copy.start())

    def receive(self, k):
        self.arrival(k).wait_recv()
        self.each(self.onward(k), lambda copy: copy.start())

    def drain(self):
        for side in range(2):
            self.each(self.own(side), lambda copy: copy.wait_send())
        for k in range(1, self.net.zs):
            self.each(self.onward(k), lambda copy: copy.wait_send())


class KeyChain(Chain):
    def __init__(self, net, buf, own, rows, sems):
        super().__init__(net, sems[0], sems[1])
        self.buf, self.mine, self.rows = buf, own, rows
        self.cs, self.cr, self.ss, self.sr = sems[2:]

    def part(self, z, c=None):
        c = self.net.c if c is None else c
        if self.rows is None:
            return self.buf.at[z, c]
        return self.buf.at[z, c, :, : self.rows]

    def swap(self, arriving=False):
        net = self.net
        dst = self.part(net.z, None if arriving else net.x)
        return remote(self.mine, dst, self.ss, self.sr, net.at(x=net.ox, c=net.oc))

    def over_c(self, k, arriving=False):
        net = self.net
        b = self.part(net.near(k), net.oc if arriving else None)
        return remote(b, b, self.cs.at[k], self.cr.at[k], net.at(c=net.oc))

    def begin(self):
        self.start()
        self.over_c(0).start()

    def pass_swap(self):
        self.swap(True).wait_recv()
        self.begin()

    def pass_z(self, k):
        self.receive(k)
        self.over_c(k).start()

    def arrived(self, k):
        self.over_c(k, True).wait_recv()

    def drain(self):
        super().drain()
        for k in range(self.net.zs):
            self.over_c(k).wait_send()


def greet(net):
    barrier = pltpu.get_barrier_semaphore()
    others = [net.at(x=net.ox), net.at(y=net.oy), net.at(c=net.oc)]
    others += [net.at(x=net.ox, c=net.oc)]
    others += [net.at(z=net.near(k)) for k in range(1, net.zs)]
    for where in others:
        pl.semaphore_signal(barrier, inc=1, device_id=where, device_id_type=pl.DeviceIdType.MESH)
    pl.semaphore_wait(barrier, len(others))


def layer_kernel(
    dims, group, scale, head_width, tok_hbm, qw_ref, kw_ref, vw_ref, ow_ref, qg_ref, kg_ref,
    out_ref, tok_ref, wkv, wq0, wq1, wo, q_ref, k_buf, v_buf, acc_ref, max_ref, att_ref,
    k_own, v_own, q_own, q_in, att_own, sum_ref, cos_ref, sin_ref, tok_sem, *sems
):
    net = Net(dims)
    rows, depth = tok_ref.shape
    pair = 2 * head_width
    kv_width = kw_ref.shape[1]
    groups = kv_width // head_width
    q_width = qw_ref.shape[1]
    width = 4 * head_width
    load = pltpu.make_async_copy(tok_hbm, tok_ref, tok_sem)
    load.start()
    me = (net.z, net.x, net.y, net.c)
    wkv[me + (slice(None), slice(0, kv_width))] = kw_ref[...]
    wkv[me + (slice(None), slice(kv_width, 2 * kv_width))] = vw_ref[...]
    half = q_width // 2
    wq0[me] = qw_ref[:, :half]
    wq1[me] = qw_ref[:, half:]
    wo[me] = ow_ref[...]
    kv_w = Gather(net, wkv, True, sems[0:8])
    q_w = [Gather(net, buf, False, sems[8 * i : 8 * i + 8]) for i, buf in ((1, wq0), (2, wq1))]
    o_w = Gather(net, wo, False, sems[24:32])
    keys = KeyChain(net, k_buf, k_own, None, sems[32:38])
    values = KeyChain(net, v_buf, v_own, head_width, sems[38:44])
    q_send, q_recv, a_send, a_recv = sems[44:]
    native = net.c == net.x
    foreign = net.c != net.x
    steps = net.zs
    greet(net)
    kv_w.start_z()
    kv_w.spread(0)
    q_w[0].spread(0)
    q_w[1].spread(0)

    lane = lax.broadcasted_iota(jnp.int32, (rows, pair), 1)
    at = lax.broadcasted_iota(jnp.int32, (rows, pair), 0) + (net.z * net.xs + net.x) * rows
    quarter = head_width // 4
    power = (lane % quarter).astype(jnp.float32) * (-math.log(rope_base) / quarter)
    spot = jnp.where(lane % head_width < 2 * quarter, at // GRID_W, at % GRID_W)
    angle = spot.astype(jnp.float32) * jnp.exp(power)
    first = lane % (2 * quarter) < quarter
    cos_ref[...] = jnp.cos(angle)
    sin_ref[...] = jnp.where(first, -jnp.sin(angle), jnp.sin(angle))

    q_ref[...] = jnp.zeros_like(q_ref)
    acc_ref[...] = jnp.zeros_like(acc_ref)
    max_ref[...] = jnp.full_like(max_ref, -jnp.inf)
    tail = v_buf.shape[3] - head_width
    v_buf[:, :, :, head_width:] = jnp.ones(v_buf.shape[:3] + (tail, rows), v_buf.dtype)
    load.wait()

    r = lax.broadcasted_iota(jnp.int32, (2 * width, width), 0) % width // head_width
    c = lax.broadcasted_iota(jnp.int32, (2 * width, width), 1) // head_width
    averager = jnp.where(r == c, 1.0 / head_width, 0.0).astype(jnp.bfloat16)
    wide_first = jnp.concatenate([first, first], axis=1)

    def twice(ref):
        return jnp.concatenate([ref[...]] * 2, axis=1)

    def product(buf, at):
        w = buf[:, :, :, :, :, at : at + width].reshape(depth, width)
        return jnp.dot(tok_ref[...], w, preferred_element_type=jnp.float32)

    def halves(t):
        high = t.astype(jnp.bfloat16)
        return high, (t - high.astype(jnp.float32)).astype(jnp.bfloat16)

    def turned(t, gain_ref):
        gain = jnp.concatenate([gain_ref[...]] * 4, axis=1)
        mean_sq = jnp.dot(
            jnp.concatenate(halves(t * t), axis=1), averager, preferred_element_type=jnp.float32
        )
        t = t * lax.rsqrt(mean_sq + epsilon) * gain
        other = jnp.where(
            wide_first, pltpu.roll(t, width - quarter, 1), pltpu.roll(t, quarter, 1)
        )
        return t * twice(cos_ref) + other * twice(sin_ref)

    for k in range(1, steps):
        kv_w.pass_z(k)
    q_w[0].start_z()
    for k in range(steps):
        kv_w.pass_x(k)
        kv_w.pass_y(k)
    q_w[1].start_z()
    for k in range(steps):
        kv_w.pass_corner(k)
    for k in range(1, steps):
        q_w[0].pass_z(k)
    q_w[0].pass_x(0)
    kv_w.finish()
    k_own[...] = turned(product(wkv, 0), kg_ref).astype(k_buf.dtype)
    v_own[...] = product(wkv, kv_width).T.astype(v_buf.dtype).reshape(v_own.shape)

    @pl.when(native)
    def _():
        k_buf[net.z, net.c] = k_own[...]
        v_buf[net.z, net.c, :, :head_width] = v_own[...]
        keys.begin()
        values.begin()

    @pl.when(foreign)
    def _():
        keys.swap().start()
        values.swap().start()

    for k in range(1, steps):
        q_w[0].pass_x(k)
    for k in range(1, steps):
        q_w[1].pass_z(k)
    for k in range(steps):
        q_w[0].pass_y(k)

    @pl.when(foreign)
    def _():
        keys.pass_swap()
        values.pass_swap()

    o_w.start_z()
    for k in range(steps):
        q_w[0].pass_corner(k)
    for k in range(steps):
        q_w[1].pass_x(k)
    o_w.spread(0)
    q_w[0].finish()

    def both(act, k):
        getattr(keys, act)(k)
        getattr(values, act)(k)

    edge = jnp.logical_or(net.z == 0, net.z == net.zs - 1)

    def early(act, inside, *where):
        @pl.when(edge != inside)
        def _():
            act(*where)

    def q_swap(g):
        return remote(
            q_own.at[g], q_in.at[g], q_send.at[g], q_recv.at[g], net.at(x=net.ox, c=net.oc)
        )

    def a_swap(g):
        return remote(
            att_own.at[g], att_ref.at[g], a_send.at[g], a_recv.at[g], net.at(x=net.ox, c=net.oc)
        )

    def project_queries(g):
        w = (wq0, wq1)[g * width // half]
        q = turned(product(w, g * width % half), qg_ref).astype(jnp.bfloat16)

        @pl.when(native)
        def _():
            q_in[g] = q

        @pl.when(foreign)
        def _():
            q_own[g] = q
            q_swap(g).start()

    def place_queries(g):
        @pl.when(foreign)
        def _():
            q_swap(g).wait_recv()

        q = (q_in[g].astype(jnp.float32) * (scale * math.log2(math.e))).T
        base = (g % 2) * head_width
        for i, part in enumerate(halves(q)):
            for n in range(group):
                q_ref[
                    g, i * pair + base : i * pair + base + head_width, n * rows : (n + 1) * rows
                ] = part[n * head_width : (n + 1) * head_width]

    def hand_on():
        for k in range(steps):
            q_w[1].pass_y(k)
        for k in range(steps):
            q_w[1].pass_corner(k)

    def later_queries():
        q_w[1].finish()
        for g in range(groups // 2, groups):
            project_queries(g)

    def place_later():
        for g in range(groups // 2, groups):
            place_queries(g)

    for g in range(groups // 2):
        project_queries(g)

    chunk = width
    keys_now = net.xs * rows
    chunks = group * rows // chunk

    def attend(k, g):
        z = net.near(k)
        k_now = k_buf[z, :, :, pl.ds(pl.multiple_of(g // 2 * pair, pair), pair)]
        k_now = k_now.reshape(keys_now, pair)
        k_now = jnp.concatenate([k_now, k_now], axis=1)
        v_now = jnp.concatenate([v_buf[z, x, g] for x in range(net.xs)], axis=1)
        cols = [slice(n * chunk, (n + 1) * chunk) for n in range(chunks)]
        scores = [
            jnp.dot(k_now, q_ref[g, :, at], preferred_element_type=jnp.float32) for at in cols
        ]
        for at, s in zip(cols, scores):
            old = max_ref[g, :, at]
            top = jnp.maximum(old, jnp.max(s, axis=0, keepdims=True))
            p = jnp.exp2(s - top).astype(v_now.dtype)
            max_ref[g, :, at] = top
            acc_ref[g, :, at] = acc_ref[g, :, at] * jnp.exp2(old - top) + jnp.dot(
                v_now, p, preferred_element_type=jnp.float32
            )

    wave = [(k, g) for k in range(steps - 1) for g in range(groups // 2)]
    late = range(groups // 2, groups)
    wave += [(k, g) for g in late for k in range(steps - 2)]
    wave += [(steps - 1, g) for g in range(groups // 2)]
    wave += [(k, g) for g in late for k in range(steps - 2, steps)]
    last = wave.index((steps - 1, 0))

    def order(t):
        at = [t == i for i in range(len(wave))]
        pick = [sum(jnp.where(hit, w[i], 0) for hit, w in zip(at, wave)) for i in range(2)]
        return pick

    events = {t: [] for t in range(steps * groups)}
    both("pass_z", 1)
    early(both, True, "pass_z", 2)
    for g in range(groups // 2):
        place_queries(g)
    both("arrived", 0)
    def only(who, act, *where):
        @pl.when(who)
        def _():
            act(*where)

    events[2].append((both, "arrived", 1))
    events[3].append((hand_on,))
    events[3].append((only, foreign, later_queries))
    for k in range(1, steps):
        events[3].append((o_w.pass_z, k))
    events[4].append((early, both, True, "pass_z", 3))
    events[4].append((only, native, later_queries))
    events[4].append((early, both, False, "pass_z", 2))
    events[4].append((both, "arrived", 2))
    events[6].append((place_later,))
    events[9].append((early, both, False, "pass_z", 3))
    events[last].append((both, "arrived", 3))
    for k in range(steps):
        events[7].append((o_w.pass_x, k))
        events[9].append((o_w.pass_y, k))
        events[12 + k].append((o_w.pass_corner, k))

    def settle(g):
        parts = []
        for n in range(group):
            cols = slice(n * rows, (n + 1) * rows)
            total = acc_ref[g, head_width : head_width + 1, cols]
            parts.append(acc_ref[g, :head_width, cols] / total)
        a = jnp.concatenate(parts, axis=0).T.astype(att_ref.dtype)

        @pl.when(native)
        def _():
            att_ref[g] = a

        @pl.when(foreign)
        def _():
            att_own[g] = a
            a_swap(g).start()

    def step(t, carry):
        k, g = order(t)
        for when, todo in events.items():
            if todo:

                @pl.when(t == when)
                def _():
                    for act, *where in todo:
                        act(*where)

        attend(k, g)

        @pl.when(k == steps - 1)
        def _():
            settle(g)

        return carry

    lax.fori_loop(0, steps * groups, step, 0)

    o_w.finish()
    across = 2 * width

    def project(first, last):
        attended = jnp.concatenate([att_ref[g] for g in range(first, last)], axis=1)
        wide = group * head_width

        def one(j, carry):
            w = wo[j, :, :, :, :, first * wide : last * wide]
            cols = pl.ds(pl.multiple_of(j * across, across), across)
            part = lax.dot_general(
                attended,
                w.reshape(across, (last - first) * wide),
                (((1,), (1,)), ((), ())),
                preferred_element_type=jnp.float32,
            )
            if last < groups:
                sum_ref[:, cols] = part
            else:
                out_ref[:, cols] = (sum_ref[:, cols] + part).astype(out_ref.dtype)
            return carry

        lax.fori_loop(0, depth // across, one, 0)

    for first, last in ((0, groups - 1), (groups - 1, groups)):

        @pl.when(foreign)
        def _():
            for g in range(first, last):
                a_swap(g).wait_recv()

        project(first, last)
    for part in (kv_w, *q_w, o_w, keys, values):
        part.drain()

    @pl.when(foreign)
    def _():
        keys.swap().wait_send()
        values.swap().wait_send()
        for g in range(groups):
            q_swap(g).wait_send()
            a_swap(g).wait_send()


def vmem():
    return pl.BlockSpec(memory_space=pltpu.VMEM)


def fast(dims, tokens, q_weight, k_weight, v_weight, out_weight, q_gain, k_gain):
    zs, xs, ys = dims
    rows_in = tokens[0]
    rows, depth = rows_in.shape
    head_width = q_gain.shape[0]
    q_width = out_weight.shape[0]
    kv_width = k_weight.shape[1]
    groups = kv_width // head_width
    group = q_width // kv_width
    pair = 2 * head_width
    own = q_weight.shape[0]
    sums = 16
    dma = pltpu.SemaphoreType.DMA
    bf16, f32 = jnp.bfloat16, jnp.float32
    gather_sems = [
        dma, dma((zs,)), dma, dma((2, zs)), dma, dma((2, zs)), dma, dma,
    ]
    key_sems = [dma((zs + 1,)), dma((zs,)), dma((zs,)), dma((zs,)), dma, dma]
    grid = (zs, xs, ys, CORES, own)
    out = pl.pallas_call(
        functools.partial(layer_kernel, dims, group, head_width ** (-0.5), head_width),
        out_shape=pltpu.VMEM((rows, depth), bf16),
        in_specs=[pl.BlockSpec(memory_space=pl.ANY)] + [vmem()] * 6,
        out_specs=vmem(),
        scratch_shapes=[
            pltpu.VMEM((rows, depth), bf16),
            pltpu.VMEM(grid + (2 * kv_width,), bf16),
            pltpu.VMEM(grid + (q_width // 2,), bf16),
            pltpu.VMEM(grid + (q_width // 2,), bf16),
            pltpu.VMEM(grid + (q_width,), bf16),
            pltpu.VMEM((groups, 2 * pair, group * rows), bf16),
            pltpu.VMEM((zs, xs, rows, kv_width), bf16),
            pltpu.VMEM((zs, xs, groups, head_width + sums, rows), bf16),
            pltpu.VMEM((groups, head_width + sums, group * rows), f32),
            pltpu.VMEM((groups, 1, group * rows), f32),
            pltpu.VMEM((groups, rows, group * head_width), bf16),
            pltpu.VMEM((rows, kv_width), bf16),
            pltpu.VMEM((groups, head_width, rows), bf16),
            pltpu.VMEM((groups, rows, group * head_width), bf16),
            pltpu.VMEM((groups, rows, group * head_width), bf16),
            pltpu.VMEM((groups, rows, group * head_width), bf16),
            pltpu.VMEM((rows, depth), f32),
            pltpu.VMEM((rows, pair), f32),
            pltpu.VMEM((rows, pair), f32),
            dma,
        ]
        + gather_sems * 4
        + key_sems * 2
        + [dma((groups,))] * 4,
        compiler_params=pltpu.CompilerParams(
            collective_id=0, has_side_effects=True, vmem_limit_bytes=VMEM_BYTES
        ),
        cost_estimate=pl.CostEstimate(
            flops=100_000_000_000, bytes_accessed=10_000_000, transcendentals=20_000_000
        ),
    )(
        rows_in, q_weight, k_weight, v_weight, out_weight.T,
        q_gain.reshape(1, head_width), k_gain.reshape(1, head_width),
    )
    return out[None]


def normalize(tensor, gain_vec):
    mean_sq = jnp.mean(tensor * tensor, axis=-1, keepdims=True)
    return tensor * lax.rsqrt(mean_sq + epsilon) * gain_vec


def rotate(tensor, offset):
    row_count = tensor.shape[0]
    head_width = tensor.shape[2]
    quarter = head_width // 4
    half_width = head_width // 2
    positions = jnp.arange(row_count, dtype=jnp.int32) + offset
    frequency = rope_base ** (-jnp.arange(quarter, dtype=jnp.float32) / quarter)

    def rotate_pair(segment, coords):
        angles = coords.astype(jnp.float32)[:, None] * frequency[None, :]
        cosine = jnp.cos(angles)[:, None, :]
        sine_val = jnp.sin(angles)[:, None, :]
        low_half = segment[..., :quarter]
        high_half = segment[..., quarter:]
        return jnp.concatenate(
            [low_half * cosine - high_half * sine_val, high_half * cosine + low_half * sine_val],
            axis=-1,
        )

    return jnp.concatenate(
        [
            rotate_pair(tensor[..., :half_width], positions // GRID_W),
            rotate_pair(tensor[..., half_width:], positions % GRID_W),
        ],
        axis=-1,
    )


def attend(query_rows, key_rows, value_rows):
    row_count, head_width = query_rows.shape
    block_rows = math.gcd(row_count, 512)
    score_scale = head_width ** (-0.5)

    def attend_block(segment):
        scores = (
            lax.dot_general(
                segment, key_rows, (((1,), (1,)), ((), ())), preferred_element_type=jnp.float32
            )
            * score_scale
        )
        row_max = jnp.max(scores, axis=-1, keepdims=True)
        weights = jnp.exp(scores - row_max)
        shares = (weights / jnp.sum(weights, axis=-1, keepdims=True)).astype(jnp.bfloat16)
        return jnp.dot(shares, value_rows, preferred_element_type=jnp.float32).astype(jnp.bfloat16)

    blocks = query_rows.reshape(row_count // block_rows, block_rows, head_width)
    return lax.map(attend_block, blocks).reshape(row_count, head_width)


def plain(tokens, q_weight, k_weight, v_weight, out_weight, q_gain, k_gain):
    rows_in = tokens[0]
    tok_count = rows_in.shape[0]
    head_width = q_gain.shape[0]
    q_width = out_weight.shape[0]
    kv_width = k_weight.shape[1]
    q_heads = q_width // head_width
    kv_heads = kv_width // head_width
    group_size = q_heads // kv_heads
    sp_count = lax.axis_size("sp")
    offset = lax.axis_index("sp") * tok_count
    weight_rows = (
        lax.all_gather(q_weight, ("sp", "dp"), axis=0, tiled=True),
        lax.all_gather(k_weight, ("sp", "dp"), axis=0, tiled=True),
        lax.all_gather(v_weight, ("sp", "dp"), axis=0, tiled=True),
    )
    query_raw, key_raw, value_raw = tuple(
        (
            jnp.dot(rows_in, rows_part, preferred_element_type=jnp.float32)
            for rows_part in weight_rows
        )
    )
    queries = rotate(
        normalize(query_raw.reshape(tok_count, q_heads, head_width), q_gain), offset
    ).astype(jnp.bfloat16)
    keys_rot = rotate(
        normalize(key_raw.reshape(tok_count, kv_heads, head_width), k_gain), offset
    ).astype(jnp.bfloat16)
    values_dev = value_raw.astype(jnp.bfloat16)
    keys_wide = jnp.broadcast_to(
        keys_rot[:, :, None, :], (tok_count, kv_heads, group_size, head_width)
    ).reshape(tok_count, q_width)
    values_wide = jnp.broadcast_to(
        values_dev.reshape(tok_count, kv_heads, 1, head_width),
        (tok_count, kv_heads, group_size, head_width),
    ).reshape(tok_count, q_width)
    q_local, k_local, v_local = (
        lax.all_to_all(
            queries.reshape(tok_count, q_width), "sp", split_axis=1, concat_axis=0, tiled=True
        ),
        lax.all_to_all(keys_wide, "sp", split_axis=1, concat_axis=0, tiled=True),
        lax.all_to_all(values_wide, "sp", split_axis=1, concat_axis=0, tiled=True),
    )
    local_heads = q_width // sp_count // head_width
    outputs = []
    for head_index in range(local_heads):
        low_col = head_index * head_width
        outputs.append(
            attend(
                q_local[:, low_col : low_col + head_width],
                k_local[:, low_col : low_col + head_width],
                v_local[:, low_col : low_col + head_width],
            )
        )
    head_results = jnp.concatenate(outputs, axis=1)
    attended = lax.all_to_all(head_results, "sp", split_axis=0, concat_axis=1, tiled=True)
    result = jnp.dot(
        attended,
        lax.all_gather(out_weight, ("sp", "dp"), axis=1, tiled=True),
        preferred_element_type=jnp.float32,
    ).astype(jnp.bfloat16)
    return result[None]


def solution(mesh):
    sp, dp = mesh.shape["sp"], mesh.shape["dp"]
    across = dp // CORES
    exchange = dp == 2 * CORES and sp % across == 0 and sp // across > 1
    body = functools.partial(fast, (sp // across, across, across)) if exchange else plain
    return jax.shard_map(
        body,
        mesh=mesh,
        in_specs=(
            P("dp", "sp", None),
            P(("sp", "dp"), None),
            P(("sp", "dp"), None),
            P(("sp", "dp"), None),
            P(None, ("sp", "dp")),
            P(),
            P(),
        ),
        out_specs=P("dp", "sp", None),
        check_vma=False,
    )
```
